32 devices in a mesh: sp: 8 (over z, y), tp: 4 (over x, core).
Axes of the slice: x: 2, y: 2, z: 4, core: 2. Of those that a mesh axis runs over, the one named last changes fastest.
Arguments:
- queries: bfloat16 [1536, 1024], P('sp', 'tp'), may hold values from -0.75 to 0.75
- key_vectors: bfloat16 [1536, 1024], P('sp', 'tp'), may hold values from -0.75 to 0.75
- values_in: bfloat16 [1536, 2048], P('sp', 'tp'), may hold values from -0.75 to 0.75
- log_decay: float32 [1536, 1024], P('sp', 'tp'), may hold values from -1 to 0
- mixed_heads: bfloat16 [1536, 2048], P('sp', 'tp'), may hold values from -6 to 6
- out_proj: bfloat16 [2048, 2048], P('tp'), may hold values from -0.125 to 0.125
- layer_input: bfloat16 [1536, 2048], P('sp'), may hold values from -6 to 6
- cotangent: bfloat16 [1536, 2048], P('sp'), may hold values from -6 to 6
- routes: int32 [1536, 2], P('sp'), may hold values from 0 to 15, all different within a row; in each aligned block of 192 rows (0 to 191, 192 to 383, ...) at most 48 rows name the same one
- route_weight: float32 [1536, 2], P('sp'), may hold values from 0.25 to 2
- gate_weight: bfloat16 [16, 2048, 1024], P('sp', None, 'tp'), may hold values from -0.125 to 0.125
- up_weight: bfloat16 [16, 2048, 1024], P('sp', None, 'tp'), may hold values from -0.125 to 0.125
- down_weight: bfloat16 [16, 1024, 2048], P('sp', 'tp'), may hold values from -0.1875 to 0.1875
Outputs:
- grad_gate: float32 [16, 2048, 1024], P('sp', None, 'tp')
- grad_up: float32 [16, 2048, 1024], P('sp', None, 'tp')
- grad_down: float32 [16, 1024, 2048], P('sp', 'tp')
- grad_proj: float32 [2048, 2048], P('sp', 'tp')
- grad_query: float32 [1536, 1024], P('sp', 'tp')
- grad_key: float32 [1536, 1024], P('sp', 'tp')
- grad_value: float32 [1536, 2048], P('sp', 'tp')
- grad_decay: float32 [1536, 1024], P('sp', 'tp')
The draws below stay inside these ranges and needn't reach their ends.
Inputs may be any that keep to these rules, and one draw needn't show every extreme that they name: `routes`: in each aligned block of 192 tokens no expert is named by more than 48 pairs, and in some block one expert is named by exactly 48 pairs; the 2 experts of a token differ.
All inputs are finite; a program needn't handle non-finite values.
Results may differ from the reference program's by a relative error of at most 0.015.
Values may be sent and summed in bfloat16 or wider, within the bound.
No kernel may reach another device: no remote copies, remote signals or barrier semaphores. Data moves between devices by JAX's collectives and lax.ppermute only.
A program may use at most 192 MiB of HBM per device.

```python
import math
import jax
import jax.numpy as jnp
import numpy as np
from jax import lax

D = 2048
HEADS = 8
DK = 128
DV = 256
FE = 1024
TOP = 2
TOK_DEV = 192
EXPERTS = 16
STREAM_LENGTH = 1536
CAP = 48
N_TP = 4


def draw_log_decay(key, part):
    lookup_entries = jax.random.split(key, 7)
    feature_total = HEADS * DK
    fast_share = 0.5
    fast = jax.random.bernoulli(lookup_entries[0], fast_share, (feature_total,))
    fast_rate = jnp.exp(jax.random.uniform(lookup_entries[1], (feature_total,), jnp.float32, jnp.log(1.0 / 50.0), jnp.log(1.0 / 30.0)))
    slow_rate = jnp.exp(jax.random.uniform(lookup_entries[2], (feature_total,), jnp.float32, jnp.log(0.05), jnp.log(0.25))) / STREAM_LENGTH
    rate = jnp.where(fast, fast_rate, slow_rate)
    blocks = STREAM_LENGTH // TOK_DEV
    block_factor = jnp.exp(jax.random.uniform(lookup_entries[3], (blocks, 1, 1), jnp.float32, -0.7, 0.7))
    rough = jnp.exp(jax.random.uniform(lookup_entries[4], (blocks, TOK_DEV, feature_total), jnp.float32, -0.4, 0.4))
    stable_mode = -(rate[None, None, :] * block_factor * rough).reshape(STREAM_LENGTH, feature_total)
    spike_location = jax.random.randint(lookup_entries[5], (3,), 0, STREAM_LENGTH)
    spike_surcharge = jax.random.uniform(lookup_entries[6], (feature_total,), jnp.float32, 0.2, 0.5)
    spike_indicator = jnp.any(jnp.arange(STREAM_LENGTH)[:, None] == spike_location[None, :], axis=1)
    return stable_mode + jnp.where(spike_indicator[:, None], jnp.log(1.0 - spike_surcharge)[None, :], 0.0)


def strengthened(entries, rng, source, target, shards_of, factor):
    owner, partner = [(jnp.arange(entries.shape[dim]) // (entries.shape[dim] // shards_of)).reshape([-1 if axis == dim else 1 for axis in range(entries.ndim)]) for dim in (source, target)]
    chosen = jax.random.permutation(rng, shards_of)[partner]
    strong = (owner == chosen) | (owner == (partner + shards_of // 2) % shards_of)
    return jnp.where(strong, factor * entries, entries)


def steps_of(key, shape, shards, smallest, high):
    def one(axis_at, shards_of):
        draws = jax.random.uniform(jax.random.fold_in(jax.random.fold_in(key, 6), axis_at), (shards_of,), jnp.float32, smallest / len(shards), high / len(shards))
        return jnp.repeat(jnp.exp(draws), shape[axis_at] // shards_of).reshape((-1,) + (1,) * (len(shape) - axis_at - 1))

    level = one(*shards[0])
    for cut in shards[1:]:
        level = level * one(*cut)
    return level


def deal_out(rng, own, number, rows, amount, top, bound, slope):
    ranking = jax.random.permutation(rng, amount)
    packed, common = shares(amount, rows * top, bound, slope, True), shares(amount, rows * top, bound, slope, False)
    places = jnp.arange(amount)

    def named(lengths, turn):
        used = int((lengths > 0).sum())
        fixed = max(1, used // 4)
        shifted = fixed + (places - fixed + turn * (used - fixed)) % max(1, amount - fixed)
        return jnp.zeros((amount,), jnp.int32).at[ranking[jnp.where(places < fixed, places, shifted)]].set(jnp.asarray(lengths, jnp.int32))

    lengths = jnp.where(number % 4 == 0, named(packed, number // 4), named(common, number - number // 4 - 1))
    mixed = jax.random.permutation(jax.random.fold_in(own, 3), amount)
    source_of, receiver = mixed[0:amount // 2 * 2:2], mixed[1:amount // 2 * 2:2]
    margin = jnp.minimum(lengths[source_of] - 1, bound - lengths[receiver]) // 2
    margin = jnp.where((source_of == ranking[0]) | (receiver == ranking[0]) | (lengths[receiver] == 0), 0, jnp.maximum(margin, 0))
    shifted = jax.random.randint(jax.random.fold_in(own, 4), (amount // 2,), 0, 1 << 20) % (margin + 1)
    lengths = lengths.at[source_of].add(-shifted).at[receiver].add(shifted)
    labels = jnp.searchsorted(jnp.cumsum(lengths), jnp.arange(rows * top), side="right").astype(jnp.int32)
    listing = labels.reshape(top, rows).T
    listing = listing[jax.random.permutation(jax.random.fold_in(own, 1), rows)]
    turn = jax.random.randint(jax.random.fold_in(own, 2), (rows, 1), 0, top)
    return jnp.take_along_axis(listing, (jnp.arange(top)[None, :] + turn) % top, axis=1)


def shares(number_of, total, limit, skew, full):
    portions = [(1 << 20) // math.isqrt(grade ** skew) + 1 for grade in range(1, number_of + 1)]
    largest = limit if full else min(limit, max(-(-total // number_of), total * portions[0] // sum(portions)))
    least = 1 if total - largest >= number_of - 1 else 0
    holding, spare = [largest] + [least] * (number_of - 1), total - largest - least * (number_of - 1)
    while spare > 0:
        free = [i for i in range(1, number_of) if holding[i] < largest] or [i for i in range(1, number_of) if holding[i] < limit]
        whole, left = sum([portions[i] for i in free]), spare
        for i in free:
            more = min(limit - holding[i], max(1, left * portions[i] // whole), spare)
            holding[i] = holding[i] + more
            spare = spare - more
    return np.array(holding)


def normal_values(key, shape, spread, limit, shards=(), kind=jnp.bfloat16):
    loudness = steps_of(key, shape, shards, -0.22, 0.18) if shards else 1.0
    values = jax.random.normal(key, shape, jnp.float32) * spread * loudness
    return jnp.minimum(jnp.maximum(values, -limit), limit).astype(kind)


def noise_with(key, dims, scale, reach, shards, heavy, kind=jnp.bfloat16):
    result = scale * jax.random.normal(key, dims, jnp.float32)
    if shards:
        result = result * steps_of(key, dims, shards, -0.22, 0.18)
    return jnp.clip(strengthened(result, jax.random.fold_in(key, 3), *heavy), -reach, reach).astype(kind)


def setup_inputs(seed: int = 0) -> dict:
    splits = jax.random.split(jax.random.key(seed), 14)
    queries = normal_values(splits[0], (STREAM_LENGTH, HEADS * DK), 0.125, 0.75, ((0, 8), (1, 4)))
    key_vectors = normal_values(splits[1], (STREAM_LENGTH, HEADS * DK), 0.125, 0.75, ((0, 8), (1, 4)))
    values_in = normal_values(splits[2], (STREAM_LENGTH, HEADS * DV), 0.125, 0.75, ((0, 8), (1, 4)))
    log_decay = draw_log_decay(jax.random.fold_in(splits[13], 71), 0)
    mixed_heads = normal_values(splits[4], (STREAM_LENGTH, HEADS * DV), 1.0, 6.0, ((0, 8), (1, 4)))
    out_proj = normal_values(splits[5], (HEADS * DV, D), (HEADS * DV) ** -0.5, 0.125, ((0, 4),))
    layer_input = normal_values(splits[6], (STREAM_LENGTH, D), 1.0, 6.0, ((0, 8),))
    cotangent = noise_with(splits[7], (STREAM_LENGTH, D), 1.0, 6.0, ((0, 8),), (0, 1, 8, 2.0))
    routes_keys = jax.random.split(jax.random.fold_in(splits[8], 1), STREAM_LENGTH // TOK_DEV)
    routes_turns = jax.random.permutation(jax.random.fold_in(splits[8], 3), STREAM_LENGTH // TOK_DEV)
    routes = jax.vmap(lambda own, number: deal_out(jax.random.fold_in(splits[8], 2), own, number, TOK_DEV, EXPERTS, TOP, CAP, 2))(routes_keys, routes_turns).reshape((STREAM_LENGTH, TOP))
    route_weight = jnp.clip(jnp.exp(math.log(2.0) - 2.0794415 * jax.random.uniform(splits[9], (STREAM_LENGTH, TOP), jnp.float32) ** steps_of(splits[9], (STREAM_LENGTH, TOP), ((0, 8),), -0.2, 0.2)), 0.25, 2.0)
    gate_weight = normal_values(splits[10], (EXPERTS, D, FE), D ** -0.5, 0.125, ((0, 8), (2, 4)))
    up_weight = normal_values(splits[11], (EXPERTS, D, FE), D ** -0.5, 0.125, ((0, 8), (2, 4)))
    down_weight = normal_values(splits[12], (EXPERTS, FE, D), FE ** -0.5, 0.1875, ((0, 8), (1, 4)))
    return dict(queries=queries, key_vectors=key_vectors, values_in=values_in, log_decay=log_decay, mixed_heads=mixed_heads, out_proj=out_proj, layer_input=layer_input, cotangent=cotangent, routes=routes, route_weight=route_weight, gate_weight=gate_weight, up_weight=up_weight, down_weight=down_weight)


def local_parts(query_f, key_f, grad_f, pair, decays):
    highest = lax.Precision.HIGHEST
    sigma = query_f.shape[2] ** -0.5
    length = query_f.shape[0]
    cum = jnp.cumsum(decays, axis=0)
    total = cum[-1]
    middle = 0.5 * total
    rise = jnp.exp(cum - middle)
    fall = jnp.exp(middle - cum)
    position = jnp.arange(length, dtype=jnp.int32)
    lower = (position[:, None] >= position[None, :])[None]
    score_fwd = jnp.where(lower, jnp.einsum("thc,shc->hts", query_f * rise, key_f * fall, precision=highest), 0.0) * sigma
    score_bwd = jnp.where(lower, 0.0, jnp.einsum("thc,shc->hts", query_f * fall, key_f * rise, precision=highest)) * sigma
    pair_fwd = jnp.where(lower, pair, 0.0)
    pair_bwd = jnp.where(lower, 0.0, pair)
    query_fwd = sigma * rise * jnp.einsum("hts,shc->thc", pair_fwd, key_f * fall, precision=highest)
    query_bwd = sigma * fall * jnp.einsum("hts,shc->thc", pair_bwd, key_f * rise, precision=highest)
    key_fwd = sigma * fall * jnp.einsum("hts,thc->shc", pair_fwd, query_f * rise, precision=highest)
    key_bwd = sigma * rise * jnp.einsum("hts,thc->shc", pair_bwd, query_f * fall, precision=highest)
    value_grad = jnp.einsum("hts,thv->shv", score_fwd + score_bwd, grad_f, precision=highest)
    return query_fwd, query_bwd, key_fwd, key_bwd, value_grad, cum, total


def state_terms(query_f, key_f, value_f, grad_f, cum, total):
    highest = lax.Precision.HIGHEST
    head_part = jnp.exp(cum)
    tail = jnp.exp(total - cum)
    kv_fwd = jnp.einsum("shc,shv->hcv", key_f * tail, value_f, precision=highest)
    qo_bwd = jnp.einsum("thc,thv->hcv", query_f * tail, grad_f, precision=highest)
    qo_fwd = jnp.einsum("thc,thv->hcv", query_f * head_part, grad_f, precision=highest)
    kv_bwd = jnp.einsum("shc,shv->hcv", key_f * head_part, value_f, precision=highest)
    return jnp.exp(total), kv_fwd, qo_bwd, qo_fwd, kv_bwd


def carried(parts, states, query_f, key_f, value_f, grad_f):
    highest = lax.Precision.HIGHEST
    sigma = query_f.shape[2] ** -0.5
    query_fwd, query_bwd, key_fwd, key_bwd, value_grad, cum, total = parts
    kv_low, qo_low, qo_high, kv_high = states
    head_part = jnp.exp(cum)
    tail = jnp.exp(total - cum)
    query_fwd = query_fwd + sigma * head_part * jnp.einsum("thv,hcv->thc", grad_f, kv_low, precision=highest)
    query_bwd = query_bwd + sigma * tail * jnp.einsum("thv,hcv->thc", grad_f, kv_high, precision=highest)
    key_fwd = key_fwd + sigma * tail * jnp.einsum("shv,hcv->shc", value_f, qo_high, precision=highest)
    key_bwd = key_bwd + sigma * head_part * jnp.einsum("shv,hcv->shc", value_f, qo_low, precision=highest)
    value_grad = value_grad + sigma * (jnp.einsum("shc,hcv->shv", key_f * tail, qo_high, precision=highest)
                                       + jnp.einsum("shc,hcv->shv", key_f * head_part, qo_low, precision=highest))
    grad_cum = query_f * (query_fwd - query_bwd) - key_f * (key_fwd - key_bwd)
    return query_fwd + query_bwd, key_fwd + key_bwd, value_grad, grad_cum


def carry_step(carry, inputs):
    decay_all, first_term, second_term = inputs
    grown = (decay_all[..., None] * carry[0] + first_term, decay_all[..., None] * carry[1] + second_term)
    return grown, carry


def expert_grads(inputs):
    rows, cots, weights, gate_w, up_w, down_w = inputs
    pre_gate = jnp.dot(rows, gate_w, preferred_element_type=jnp.float32)
    pre_up = jnp.dot(rows, up_w, preferred_element_type=jnp.float32)
    weighted = (weights[:, None] * cots.astype(jnp.float32)).astype(jnp.bfloat16)
    d_act = jnp.dot(weighted, down_w.T, preferred_element_type=jnp.float32)
    sigmoid_gate = jax.nn.sigmoid(pre_gate)
    silu_gate = pre_gate * sigmoid_gate
    act = (silu_gate * pre_up).astype(jnp.bfloat16)
    d_gate = (d_act * pre_up * sigmoid_gate * (1.0 + pre_gate * (1.0 - sigmoid_gate))).astype(jnp.bfloat16)
    d_up = (d_act * silu_gate).astype(jnp.bfloat16)
    grad_down = jnp.dot(act.T, weighted, preferred_element_type=jnp.float32)
    grad_gate = jnp.dot(rows.T, d_gate, preferred_element_type=jnp.float32)
    grad_up = jnp.dot(rows.T, d_up, preferred_element_type=jnp.float32)
    part_width = FE // N_TP
    parts = jnp.einsum("rpf,pfd->rpd", d_gate.reshape(-1, N_TP, part_width).astype(jnp.float32),
                       gate_w.T.reshape(N_TP, part_width, D).astype(jnp.float32))
    parts = parts + jnp.einsum("rpf,pfd->rpd", d_up.reshape(-1, N_TP, part_width).astype(jnp.float32),
                               up_w.T.reshape(N_TP, part_width, D).astype(jnp.float32))
    rounded = lax.optimization_barrier(parts.astype(jnp.bfloat16))
    row_grad = jnp.sum(rounded.astype(jnp.float32), axis=1).astype(jnp.bfloat16)
    return grad_gate, grad_up, grad_down, row_grad


def reference(queries, key_vectors, values_in, log_decay, mixed_heads, out_proj, layer_input, cotangent,
              routes, route_weight, gate_weight, up_weight, down_weight):
    blocks = STREAM_LENGTH // TOK_DEV
    rows_all = blocks * CAP
    flat_route = routes.reshape(blocks, TOK_DEV * TOP)
    onehot = (flat_route[:, :, None] == jnp.arange(EXPERTS, dtype=jnp.int32)[None, None, :]).astype(jnp.int32)
    rank = jnp.sum((jnp.cumsum(onehot, axis=1) - onehot) * onehot, axis=2)
    block_id = jnp.arange(blocks, dtype=jnp.int32)[:, None]
    place = (flat_route * rows_all + block_id * CAP + rank).reshape(-1).astype(jnp.int32)
    token_id = jnp.arange(STREAM_LENGTH * TOP, dtype=jnp.int32) // TOP
    slot_token = jnp.zeros((EXPERTS * rows_all,), jnp.int32).at[place].set(token_id)
    filled = jnp.zeros((EXPERTS * rows_all,), jnp.float32).at[place].set(1.0)
    slot_weight = jnp.zeros((EXPERTS * rows_all,), jnp.float32).at[place].set(route_weight.reshape(-1))
    expert_rows = (layer_input[slot_token].astype(jnp.float32) * filled[:, None]).astype(jnp.bfloat16)
    expert_cot = (cotangent[slot_token].astype(jnp.float32) * filled[:, None]).astype(jnp.bfloat16)
    grad_gate, grad_up, grad_down, row_grad = lax.map(expert_grads, (
        expert_rows.reshape(EXPERTS, rows_all, D), expert_cot.reshape(EXPERTS, rows_all, D),
        slot_weight.reshape(EXPERTS, rows_all), gate_weight, up_weight, down_weight))
    back = row_grad.reshape(EXPERTS * rows_all, D)[place].reshape(STREAM_LENGTH, TOP, D)
    token_grad = (cotangent.astype(jnp.float32) + jnp.sum(back.astype(jnp.float32), axis=1)).astype(jnp.bfloat16)
    grad_proj = jnp.dot(token_grad.T, mixed_heads, preferred_element_type=jnp.float32)
    head_grad = jnp.dot(token_grad, out_proj.T, preferred_element_type=jnp.float32)

    highest = lax.Precision.HIGHEST
    query_f = queries.astype(jnp.float32).reshape(blocks, TOK_DEV, HEADS, DK)
    key_f = key_vectors.astype(jnp.float32).reshape(blocks, TOK_DEV, HEADS, DK)
    value_f = values_in.astype(jnp.float32).reshape(blocks, TOK_DEV, HEADS, DV)
    grad_f = head_grad.reshape(blocks, TOK_DEV, HEADS, DV)
    decays = log_decay.reshape(blocks, TOK_DEV, HEADS, DK)
    pair = jnp.einsum("bthv,bshv->bhts", grad_f, value_f, precision=highest)
    parts = jax.vmap(local_parts)(query_f, key_f, grad_f, pair, decays)
    terms = jax.vmap(state_terms)(query_f, key_f, value_f, grad_f, parts[5], parts[6])
    zeros = jnp.zeros((HEADS, DK, DV), jnp.float32)
    _, low = lax.scan(carry_step, (zeros, zeros), (terms[0], terms[1], terms[2]))
    _, high = lax.scan(carry_step, (zeros, zeros), (terms[0], terms[3], terms[4]), reverse=True)
    query_grad, key_grad, value_grad, grad_cum = jax.vmap(carried)(
        parts, (low[0], low[1], high[0], high[1]), query_f, key_f, value_f, grad_f)
    grad_cum = grad_cum.reshape(STREAM_LENGTH, HEADS * DK)
    grad_decay = jnp.flip(jnp.cumsum(jnp.flip(grad_cum, 0), axis=0), 0)
    return (grad_gate, grad_up, grad_down, grad_proj, query_grad.reshape(STREAM_LENGTH, HEADS * DK),
            key_grad.reshape(STREAM_LENGTH, HEADS * DK), value_grad.reshape(STREAM_LENGTH, HEADS * DV), grad_decay)
```

```python
import functools
import jax
import jax.numpy as jnp
from jax import lax
from jax.experimental import pallas as pl
from jax.experimental.pallas import tpu as pltpu
from jax.sharding import PartitionSpec as P

DK = 128
DV = 256
BF = jnp.bfloat16
F32 = jnp.float32


def flip_bit(value, axis, bit):
    size = lax.axis_size(axis)
    return lax.ppermute(value, axis, [(s, s ^ bit) for s in range(size)])


def shift_pairs(value, distance, forward):
    size = lax.axis_size("sp")
    step = 2 * distance if forward else size - 2 * distance
    return lax.ppermute(value, "sp", [(s, (s + step) % size) for s in range(size)])


def mm(a, b, contract):
    return lax.dot_general(
        a.astype(BF), b.astype(BF), ((contract[0], contract[1]), ((), ())), preferred_element_type=F32
    )


NN = ((1,), (0,))
NT = ((1,), (1,))
TN = ((0,), (0,))


def lower_mask(length, strict=False):
    row = lax.broadcasted_iota(jnp.int32, (length, length), 0)
    col = lax.broadcasted_iota(jnp.int32, (length, length), 1)
    return row > col if strict else row >= col


def head_cols(h, width):
    return slice(h * width, (h + 1) * width)


def early_kernel(q_ref, k_ref, v_ref, ld_ref, cum_ref, score_ref, kvf_ref, kvb_ref):
    length = q_ref.shape[0]
    heads = q_ref.shape[1] // DK
    sigma = DK ** (-0.5)
    tri = jnp.where(lower_mask(length), 1.0, 0.0).astype(F32)
    upper = jnp.logical_not(lower_mask(length, True))
    for h in range(heads):
        ch = head_cols(h, DK)
        cum = jnp.dot(
            tri, ld_ref[:, ch], precision=lax.Precision.HIGHEST, preferred_element_type=F32
        )
        cum_ref[:, ch] = cum
        total = cum[length - 1 :, :]
        middle = 0.5 * total
        rise = jnp.exp(cum - middle)
        fall = jnp.exp(middle - cum)
        qf = q_ref[:, ch].astype(F32)
        kf = k_ref[:, ch].astype(F32)
        ahead = mm(kf * fall, qf * rise, NT)
        behind = mm(kf * rise, qf * fall, NT)
        score_ref[h] = (jnp.where(upper, ahead, behind) * sigma).astype(BF)
        vv = v_ref[:, head_cols(h, DV)]
        kvf_ref[h] = mm(vv, kf * jnp.exp(total - cum), TN)
        kvb_ref[h] = mm(vv, kf * jnp.exp(cum), TN)


def grad_kernel(tg_ref, w_ref, q_ref, cum_ref, o_ref, qof_ref, qob_ref):
    length = q_ref.shape[0]
    heads = q_ref.shape[1] // DK
    for h in range(heads):
        ch = head_cols(h, DK)
        vh = head_cols(h, DV)
        out = mm(tg_ref[...], w_ref[vh, :], NT)
        o_ref[:, vh] = out.astype(BF)
        cum = cum_ref[:, ch]
        total = cum[length - 1 :, :]
        qf = q_ref[:, ch].astype(F32)
        qof_ref[h] = mm(out, qf * jnp.exp(total - cum), TN)
        qob_ref[h] = mm(out, qf * jnp.exp(cum), TN)


def local_kernel(
    q_ref, k_ref, v_ref, cum_ref, o_ref, score_ref, kvl_ref, kvh_ref,
    gq_ref, dq_ref, kf_ref, kb_ref, vg_ref,
):
    length = q_ref.shape[0]
    heads = q_ref.shape[1] // DK
    sigma = DK ** (-0.5)
    lower = lower_mask(length)
    for h in range(heads):
        ch = head_cols(h, DK)
        vh = head_cols(h, DV)
        cum = cum_ref[:, ch]
        total = cum[length - 1 :, :]
        middle = 0.5 * total
        rise = jnp.exp(cum - middle)
        fall = jnp.exp(middle - cum)
        qf = q_ref[:, ch].astype(F32)
        kf = k_ref[:, ch].astype(F32)
        oo = o_ref[:, vh]
        vv = v_ref[:, vh]
        pair = mm(oo, vv, NT)
        fwd = jnp.where(lower, pair, 0.0).astype(BF)
        bwd = jnp.where(lower, 0.0, pair).astype(BF)
        q_fwd = rise * mm(fwd, kf * fall, NN) + jnp.exp(cum) * mm(oo, kvl_ref[h], NN)
        q_bwd = fall * mm(bwd, kf * rise, NN) + jnp.exp(total - cum) * mm(oo, kvh_ref[h], NN)
        gq_ref[:, ch] = sigma * (q_fwd + q_bwd)
        dq_ref[:, ch] = qf * (sigma * (q_fwd - q_bwd))
        kf_ref[:, ch] = fall * mm(fwd, qf * rise, TN)
        kb_ref[:, ch] = rise * mm(bwd, qf * fall, TN)
        vg_ref[:, vh] = mm(score_ref[h], oo, NN)


def final_kernel(
    k_ref, v_ref, cum_ref, dq_ref, kf_ref, kb_ref, vg_ref, qol_ref, qoh_ref, bey_ref,
    gk_ref, gv_ref, gd_ref,
):
    length = k_ref.shape[0]
    heads = k_ref.shape[1] // DK
    sigma = DK ** (-0.5)
    suffix = jnp.where(lower_mask(length, True), 0.0, 1.0).astype(F32)
    for h in range(heads):
        ch = head_cols(h, DK)
        vh = head_cols(h, DV)
        cum = cum_ref[:, ch]
        total = cum[length - 1 :, :]
        ahead = jnp.exp(cum)
        tail = jnp.exp(total - cum)
        kf = k_ref[:, ch].astype(F32)
        vv = v_ref[:, vh]
        high = qoh_ref[h].astype(BF)
        low = qol_ref[h].astype(BF)
        k_fwd = kf_ref[:, ch] + tail * mm(vv, high, NN)
        k_bwd = kb_ref[:, ch] + ahead * mm(vv, low, NN)
        gk_ref[:, ch] = sigma * (k_fwd + k_bwd)
        gv_ref[:, vh] = vg_ref[:, vh] + sigma * (mm(kf * tail, high, NT) + mm(kf * ahead, low, NT))
        change = dq_ref[:, ch] - kf * (sigma * (k_fwd - k_bwd))
        gd_ref[:, ch] = bey_ref[h] + jnp.dot(
            suffix, change, precision=lax.Precision.HIGHEST, preferred_element_type=F32
        )


def call(kernel, outs, *args):
    return pl.pallas_call(kernel, out_shape=[jax.ShapeDtypeStruct(s, d) for s, d in outs])(*args)


def scan_states(ahead, back, decays=None, total=None):
    size = lax.axis_size("sp")
    place = lax.axis_index("sp")
    steps = size.bit_length() - 1
    rows = ahead.shape[1]
    low = jnp.zeros_like(ahead)
    high = jnp.zeros_like(back)
    record = []
    if decays is None:
        group, below, above = total, jnp.zeros_like(total), jnp.zeros_like(total)
    for k in range(steps):
        upper = ((place >> k) & 1) == 1
        last = k == steps - 1
        if decays is None:
            other = jnp.zeros_like(group) if last else flip_bit(group, "sp", 1 << k)
            record.append((jnp.exp(group), jnp.exp(other), jnp.exp(below), jnp.exp(above)))
            below = below + jnp.where(upper, other, 0.0)
            above = above + jnp.where(upper, 0.0, other)
            group = group + other
            mine, theirs, under, over = record[-1]
        else:
            mine, theirs, under, over = decays[k]
        if last:
            sent = jnp.where(upper, back, ahead).astype(BF)
            got = flip_bit(sent, "sp", 1 << k).astype(F32)
            got_ahead = got_back = got
        else:
            sent = jnp.concatenate([ahead.astype(BF), back.astype(BF)], axis=1)
            got = flip_bit(sent, "sp", 1 << k).astype(F32)
            got_ahead, got_back = got[:, :rows], got[:, rows:]
        low = jnp.where(upper, low + under * got_ahead, low)
        high = jnp.where(upper, high, high + over * got_back)
        if not last:
            ahead, back = (
                jnp.where(upper, mine * got_ahead + ahead, theirs * ahead + got_ahead),
                jnp.where(upper, got_back + theirs * back, back + mine * got_back),
            )
    return low, high, (decays if decays is not None else record)


def body(
    queries,
    key_vectors,
    values_in,
    log_decay,
    mixed_heads,
    out_proj,
    layer_input,
    cotangent,
    routes,
    route_weight,
    gate_weight,
    up_weight,
    down_weight,
):
    tokens, top = routes.shape
    seq = lax.axis_size("sp")
    tensor = lax.axis_size("tp")
    halves = seq // 2
    experts = gate_weight.shape[0]
    all_experts = experts * seq
    cap = 2 * tokens * top // all_experts
    width = cotangent.shape[1]
    part = width // tensor
    place_sp = lax.axis_index("sp")
    place_tp = lax.axis_index("tp")
    side = (place_tp >> 1) & 1
    core = place_tp & 1
    my_low = place_sp & 1
    my_high = place_sp >> 1

    flat_route = routes.reshape(-1)
    onehot = flat_route[:, None] == jnp.arange(all_experts, dtype=jnp.int32)[None, :]
    before = lax.dot_general(
        lower_mask(tokens * top, True).astype(BF),
        onehot.astype(BF),
        (((1,), (0,)), ((), ())),
        preferred_element_type=F32,
    )
    rank = jnp.sum(jnp.where(onehot, before, 0.0), axis=1).astype(jnp.int32)
    owner = flat_route // experts
    parity = (owner & 1) ^ my_low
    distance = ((owner >> 1) - my_high) % halves
    slot = ((parity * halves + distance) * experts + flat_route % experts) * cap + rank
    slot = slot.reshape(tokens, top)
    slots = seq * experts * cap
    numbers = lax.broadcasted_iota(jnp.int32, (slots, tokens), 0)
    taken = [slot[:, k][None, :] == numbers for k in range(top)]
    pick = functools.reduce(jnp.logical_or, taken).astype(BF)
    slot_weight = functools.reduce(
        jnp.add,
        [jnp.sum(jnp.where(taken[k], route_weight[:, k][None, :], 0.0), axis=1) for k in range(top)],
    )
    own_input = lax.dynamic_slice_in_dim(layer_input, place_tp * part, part, 1)
    own_cot = lax.dynamic_slice_in_dim(cotangent, place_tp * part, part, 1)
    sent_rows = lax.dot_general(pick, own_input, (((1,), (0,)), ((), ()))).astype(BF)
    sent_cot = lax.dot_general(
        pick, own_cot, (((1,), (0,)), ((), ())), preferred_element_type=F32
    )
    sent_weighted = (slot_weight[:, None] * sent_cot).astype(BF)

    def dispatch(rows):
        rows = rows.reshape(2, halves, experts * cap, part)
        swapped = flip_bit(rows[1], "sp", 1)
        chunks = []
        for d in range(halves):
            chunk = jnp.concatenate([rows[0, d], swapped[d]], axis=0)
            if d:
                chunk = shift_pairs(chunk, d, True)
            chunks.append(chunk)
        crossed = [flip_bit(chunk, "tp", 2) for chunk in chunks]
        own = jnp.stack(chunks)
        far = jnp.stack(crossed)
        pair = jnp.stack([jnp.where(side == 0, own, far), jnp.where(side == 0, far, own)])
        other = flip_bit(pair, "tp", 1)
        first = jnp.where(core == 0, pair, other)
        second = jnp.where(core == 0, other, pair)
        full = jnp.concatenate([first[0], second[0], first[1], second[1]], axis=2)
        full = full.reshape(halves, 2, experts, cap, width)
        return full.transpose(2, 0, 1, 3, 4).reshape(experts, halves * 2 * cap, width)

    expert_rows = dispatch(sent_rows)
    weighted = dispatch(sent_weighted)

    heads = queries.shape[1] // DK
    state = ((heads, DV, DK), F32)
    key_shape = ((tokens, heads * DK), F32)
    value_shape = ((tokens, heads * DV), F32)
    cum, score, kv_ahead, kv_back = call(
        early_kernel,
        [key_shape, ((heads, tokens, tokens), BF), state, state],
        queries, key_vectors, values_in, log_decay,
    )
    total = cum[tokens - 1].reshape(heads, 1, DK)
    kv_low, kv_high, decays = scan_states(kv_ahead, kv_back, total=total)
    mixed = [mixed_heads] + [shift_pairs(mixed_heads, d, True) for d in range(1, halves)]

    pre_gate = jnp.einsum("erd,edf->erf", expert_rows, gate_weight, preferred_element_type=F32)
    pre_up = jnp.einsum("erd,edf->erf", expert_rows, up_weight, preferred_element_type=F32)
    d_act = jnp.einsum("erd,efd->erf", weighted, down_weight, preferred_element_type=F32)
    sigmoid_gate = jax.nn.sigmoid(pre_gate)
    silu_gate = pre_gate * sigmoid_gate
    act = (silu_gate * pre_up).astype(BF)
    d_gate = (d_act * pre_up * sigmoid_gate * (1.0 + pre_gate * (1.0 - sigmoid_gate))).astype(BF)
    d_up = (d_act * silu_gate).astype(BF)
    partial_value = jnp.einsum(
        "erf,edf->erd", d_gate, gate_weight, preferred_element_type=F32
    ) + jnp.einsum("erf,edf->erd", d_up, up_weight, preferred_element_type=F32)
    grad_gate = jnp.einsum("erd,erf->edf", expert_rows, d_gate, preferred_element_type=F32)
    grad_up = jnp.einsum("erd,erf->edf", expert_rows, d_up, preferred_element_type=F32)
    grad_down = jnp.einsum("erf,erd->efd", act, weighted, preferred_element_type=F32)

    value = partial_value.astype(BF).reshape(experts, halves, 2, cap, 2, 2, part)
    value = value.transpose(4, 5, 1, 2, 0, 3, 6)
    by_core = jnp.where(core == 0, value[:, 0], value[:, 1])
    for_core = jnp.where(core == 0, value[:, 1], value[:, 0])
    by_core = (by_core.astype(F32) + flip_bit(for_core, "tp", 1).astype(F32)).astype(BF)
    by_side = jnp.where(side == 0, by_core[0], by_core[1])
    for_side = jnp.where(side == 0, by_core[1], by_core[0])
    returned = []
    for d in range(halves):
        row = by_side[d].astype(F32) + flip_bit(for_side[d], "tp", 2).astype(F32)
        row = row.astype(BF)
        returned.append(shift_pairs(row, d, False) if d else row)
    returned = jnp.stack(returned)
    same, other = returned[:, 0], flip_bit(returned[:, 1], "sp", 1)
    rows_back = jnp.stack([same, other]).reshape(slots, part)
    gathered = lax.dot_general(
        pick, rows_back, (((0,), (0,)), ((), ())), preferred_element_type=F32
    )
    token_part = (own_cot.astype(F32) + gathered).astype(BF)
    far = flip_bit(token_part, "tp", 2)
    pair = jnp.stack([jnp.where(side == 0, token_part, far), jnp.where(side == 0, far, token_part)])
    other = flip_bit(pair, "tp", 1)
    first = jnp.where(core == 0, pair, other)
    second = jnp.where(core == 0, other, pair)
    token_grad = jnp.concatenate([first[0], second[0], first[1], second[1]], axis=1)

    out_bf, qo_ahead, qo_back = call(
        grad_kernel,
        [((tokens, heads * DV), BF), state, state],
        token_grad, out_proj, queries, cum,
    )
    qo_low, qo_high, _ = scan_states(qo_ahead, qo_back, decays=decays)
    query_grad, dq, k_fwd, k_bwd, v_local = call(
        local_kernel,
        [key_shape, key_shape, key_shape, key_shape, value_shape],
        queries, key_vectors, values_in, cum, out_bf, score, kv_low, kv_high,
    )
    decay_all = jnp.exp(total)
    beyond = (DK ** (-0.5)) * jnp.sum(
        qo_high * (decay_all * kv_low + kv_ahead) + kv_high * (decay_all * qo_low + qo_ahead),
        axis=1,
        keepdims=True,
    )
    key_grad, value_grad, grad_decay = call(
        final_kernel,
        [key_shape, value_shape, key_shape],
        key_vectors, values_in, cum, dq, k_fwd, k_bwd, v_local, qo_low, qo_high, beyond,
    )

    feats = width // halves
    cut = [
        lax.dynamic_slice_in_dim(token_grad, ((my_high + d) % halves) * feats, feats, 1)
        for d in range(halves)
    ]
    cut = [shift_pairs(c, d, True) if d else c for d, c in enumerate(cut)]
    block = lax.dot_general(
        jnp.concatenate(cut), jnp.concatenate(mixed), (((0,), (0,)), ((), ())),
        preferred_element_type=F32,
    ).reshape(2, feats // 2, -1)
    keep = jnp.where(my_low == 0, block[0], block[1])
    give = jnp.where(my_low == 0, block[1], block[0])
    grad_proj = keep + flip_bit(give, "sp", 1)
    return (
        grad_gate,
        grad_up,
        grad_down,
        grad_proj,
        query_grad,
        key_grad,
        value_grad,
        grad_decay,
    )


def solution(mesh):
    return jax.shard_map(
        body,
        mesh=mesh,
        in_specs=(
            P("sp", "tp"),
            P("sp", "tp"),
            P("sp", "tp"),
            P("sp", "tp"),
            P("sp", "tp"),
            P("tp", None),
            P("sp", None),
            P("sp", None),
            P("sp", None),
            P("sp", None),
            P("sp", None, "tp"),
            P("sp", None, "tp"),
            P("sp", "tp", None),
        ),
        out_specs=(
            P("sp", None, "tp"),
            P("sp", None, "tp"),
            P("sp", "tp", None),
            P("sp", "tp"),
            P("sp", "tp"),
            P("sp", "tp"),
            P("sp", "tp"),
            P("sp", "tp"),
        ),
        check_vma=False,
    )
```

```python
import functools
import jax
import jax.numpy as jnp
from jax import lax
from jax.experimental import pallas as pl
from jax.experimental.pallas import tpu as pltpu
from jax.sharding import PartitionSpec as P

DK = 128
DV = 256
BF = jnp.bfloat16
F32 = jnp.float32


def flip_bit(value, axis, bit):
    size = lax.axis_size(axis)
    return lax.ppermute(value, axis, [(s, s ^ bit) for s in range(size)])


def shift(value, step):
    size = lax.axis_size("sp")
    return lax.ppermute(value, "sp", [(s, (s + step) % size) for s in range(size)])


def distances(size):
    return sorted(range(1, size), key=lambda d: abs(d - size // 2))


def message_groups(size):
    order = distances(size)
    order = [order[0], 0] + order[1:]
    step = max(1, size // 4)
    return [order[i : i + step] for i in range(0, size, step)]


def mm(a, b, contract):
    return lax.dot_general(
        a.astype(BF), b.astype(BF), ((contract[0], contract[1]), ((), ())), preferred_element_type=F32
    )


NN = ((1,), (0,))
NT = ((1,), (1,))
TN = ((0,), (0,))


def lower_mask(length, strict=False):
    row = lax.broadcasted_iota(jnp.int32, (length, length), 0)
    col = lax.broadcasted_iota(jnp.int32, (length, length), 1)
    return row > col if strict else row >= col


def head_cols(h, width):
    return slice(h * width, (h + 1) * width)


def early_kernel(q_ref, k_ref, v_ref, ld_ref, cum_ref, score_ref, kvf_ref, kvb_ref, send_ref):
    length = q_ref.shape[0]
    heads = q_ref.shape[1] // DK
    sigma = DK ** (-0.5)
    tri = jnp.where(lower_mask(length), 1.0, 0.0).astype(F32)
    upper = jnp.logical_not(lower_mask(length, True))
    for h in range(heads):
        ch = head_cols(h, DK)
        cum = jnp.dot(
            tri, ld_ref[:, ch], precision=lax.Precision.HIGHEST, preferred_element_type=F32
        )
        cum_ref[:, ch] = cum
        total = cum[length - 1 :, :]
        middle = 0.5 * total
        rise = jnp.exp(cum - middle)
        fall = jnp.exp(middle - cum)
        qf = q_ref[:, ch].astype(F32)
        kf = k_ref[:, ch].astype(F32)
        ahead = mm(kf * fall, qf * rise, NT)
        behind = mm(kf * rise, qf * fall, NT)
        score_ref[h] = (jnp.where(upper, ahead, behind) * sigma).astype(BF)
        vv = v_ref[:, head_cols(h, DV)]
        ahead = mm(vv, kf * jnp.exp(total - cum), TN)
        back = mm(vv, kf * jnp.exp(cum), TN)
        kvf_ref[h] = ahead
        kvb_ref[h] = back
        send_ref[h, :DV, :] = ahead.astype(BF)
        send_ref[h, DV:, :] = back.astype(BF)


def slot_kernel(base_ref, route_ref, slot_ref, *, experts_all):
    top, tokens = base_ref.shape
    names = lax.broadcasted_iota(jnp.int32, (experts_all, tokens), 0)
    hits = [route_ref[k : k + 1, :] == names for k in range(top)]
    count = functools.reduce(jnp.add, [jnp.where(hit, 1.0, 0.0) for hit in hits]).astype(BF)
    row = lax.broadcasted_iota(jnp.int32, (tokens, tokens), 0)
    col = lax.broadcasted_iota(jnp.int32, (tokens, tokens), 1)
    before = mm(count, jnp.where(row < col, 1.0, 0.0), NN)
    for k in range(top):
        rank = jnp.sum(jnp.where(hits[k], before, 0.0), axis=0, keepdims=True)
        slot_ref[k : k + 1, :] = base_ref[k : k + 1, :] + rank.astype(jnp.int32)


def picked(slot_ref, first, rows):
    top, tokens = slot_ref.shape
    numbers = first + lax.broadcasted_iota(jnp.int32, (rows, tokens), 0)
    return [slot_ref[k : k + 1, :] == numbers for k in range(top)]


def pick_kernel(place_ref, base_ref, route_ref, weight_ref, in_ref, cot_ref, slot_ref, *outs, experts_all):
    slot_kernel(base_ref, route_ref, slot_ref, experts_all=experts_all)
    _, rows, part = outs[0].shape
    lanes = pl.ds(pl.multiple_of(place_ref[0] * part, part), part)
    own_in = in_ref[:, lanes]
    own_cot = cot_ref[:, lanes]
    for d, out in enumerate(outs):
        hits = picked(slot_ref, d * rows, rows)
        pick = jnp.where(functools.reduce(jnp.logical_or, hits), 1.0, 0.0).astype(BF)
        scale = functools.reduce(
            jnp.add,
            [
                jnp.sum(jnp.where(hit, weight_ref[k : k + 1, :], 0.0), axis=1, keepdims=True)
                for k, hit in enumerate(hits)
            ],
        )
        out[0] = mm(pick, own_in, NN).astype(BF)
        out[1] = (scale * mm(pick, own_cot, NN)).astype(BF)


def join_kernel(place_ref, slot_ref, cot_ref, *refs):
    part_ref = refs[-1]
    rows, part = refs[0].shape
    total = cot_ref[:, pl.ds(pl.multiple_of(place_ref[0] * part, part), part)].astype(F32)
    for d, ref in enumerate(refs[:-1]):
        hits = picked(slot_ref, d * rows, rows)
        pick = jnp.where(functools.reduce(jnp.logical_or, hits), 1.0, 0.0).astype(BF)
        total = total + mm(pick, ref[...], TN)
    part_ref[...] = total.astype(BF)


def piece(refs, tensor, r, array, e, cap):
    blocks = []
    for ref in refs[r::tensor]:
        for i in range(ref.shape[0]):
            blocks.append(ref[i, array, e * cap : (e + 1) * cap, :])
    return jnp.concatenate(blocks, axis=0)


def expert_kernel(place_ref, *refs, tensor, cap, count):
    pieces = refs[:count]
    gate_ref, up_ref, down_ref = refs[count : count + 3]
    values = refs[count + 3 : -3]
    act_ref, dg_ref, du_ref = refs[-3:]
    experts, _, part, _ = gate_ref.shape
    for e in range(experts):
        gate = up = d_act = None
        for r in range(tensor):
            q = place_ref[0] ^ r
            rows = piece(pieces, tensor, r, 0, e, cap)
            g = mm(rows, gate_ref[e, q], NN)
            u = mm(rows, up_ref[e, q], NN)
            lanes = pl.ds(pl.multiple_of(q * part, part), part)
            a = mm(piece(pieces, tensor, r, 1, e, cap), down_ref[e, :, lanes], NT)
            gate, up, d_act = (g, u, a) if r == 0 else (gate + g, up + u, d_act + a)
        s = 1.0 / (1.0 + jnp.exp(-gate))
        silu = gate * s
        act_ref[e] = (silu * up).astype(BF)
        dg = (d_act * up * s * (1.0 + gate * (1.0 - s))).astype(BF)
        du = (d_act * silu).astype(BF)
        dg_ref[e] = dg
        du_ref[e] = du
        for r in range(tensor):
            q = place_ref[0] ^ r
            value = (mm(dg, gate_ref[e, q], NT) + mm(du, up_ref[e, q], NT)).astype(BF)
            at = 0
            for ref in values[r::tensor]:
                for i in range(ref.shape[0]):
                    ref[i, e * cap : (e + 1) * cap, :] = value[at : at + cap, :]
                    at += cap


def rows_kernel(place_ref, *refs, tensor, cap):
    dg_ref, du_ref, gg_ref, gu_ref = refs[-4:]
    pieces = refs[:-4]
    for r in range(tensor):

        @pl.when(pl.program_id(0) == r)
        def _():
            for e in range(gg_ref.shape[0]):
                rows = piece(pieces, tensor, r, 0, e, cap)
                gg_ref[e] = mm(rows, dg_ref[e], TN)
                gu_ref[e] = mm(rows, du_ref[e], TN)


def weighted_kernel(place_ref, *refs, tensor, cap):
    act_ref, gd_ref = refs[-2:]
    pieces = refs[:-2]
    for r in range(tensor):

        @pl.when(pl.program_id(0) == r)
        def _():
            for e in range(gd_ref.shape[0]):
                gd_ref[e] = mm(act_ref[e], piece(pieces, tensor, r, 0, e, cap), TN)


def grad_kernel(place_ref, *refs, tensor):
    parts = refs[:tensor]
    w_ref, q_ref, cum_ref, o_ref, send_ref, qof_ref, qob_ref = refs[tensor:]
    length = q_ref.shape[0]
    heads = q_ref.shape[1] // DK
    part = parts[0].shape[1]
    for h in range(heads):
        ch = head_cols(h, DK)
        vh = head_cols(h, DV)
        out = None
        for r in range(tensor):
            lanes = pl.ds(pl.multiple_of((place_ref[0] ^ r) * part, part), part)
            term = mm(parts[r][...], w_ref[vh, lanes], NT)
            out = term if r == 0 else out + term
        o_ref[:, vh] = out.astype(BF)
        cum = cum_ref[:, ch]
        total = cum[length - 1 :, :]
        qf = q_ref[:, ch].astype(F32)
        ahead = mm(out, qf * jnp.exp(total - cum), TN)
        back = mm(out, qf * jnp.exp(cum), TN)
        qof_ref[h] = ahead
        qob_ref[h] = back
        send_ref[h, :DV, :] = ahead.astype(BF)
        send_ref[h, DV:, :] = back.astype(BF)


def local_kernel(
    flag_ref, q_ref, k_ref, v_ref, cum_ref, o_ref, score_ref, low_ref, high_ref, got_ref, *refs
):
    decay_refs = refs[:4]
    gq_ref, dq_ref, kf_ref, kb_ref, vg_ref, kvl_ref, kvh_ref = refs[4:]
    length = q_ref.shape[0]
    heads = q_ref.shape[1] // DK
    sigma = DK ** (-0.5)
    lower = lower_mask(length)
    for h in range(heads):
        ch = head_cols(h, DK)
        vh = head_cols(h, DV)
        cum = cum_ref[:, ch]
        total = cum[length - 1 :, :]
        middle = 0.5 * total
        rise = jnp.exp(cum - middle)
        fall = jnp.exp(middle - cum)
        qf = q_ref[:, ch].astype(F32)
        kf = k_ref[:, ch].astype(F32)
        oo = o_ref[:, vh]
        vv = v_ref[:, vh]
        pair = mm(oo, vv, NT)
        fwd = jnp.where(lower, pair, 0.0).astype(BF)
        bwd = jnp.where(lower, 0.0, pair).astype(BF)
        kv_low, kv_high = close(flag_ref, low_ref, high_ref, got_ref, decay_refs, h)
        kvl_ref[h] = kv_low
        kvh_ref[h] = kv_high
        q_fwd = rise * mm(fwd, kf * fall, NN) + jnp.exp(cum) * mm(oo, kv_low, NN)
        q_bwd = fall * mm(bwd, kf * rise, NN) + jnp.exp(total - cum) * mm(oo, kv_high, NN)
        gq_ref[:, ch] = sigma * (q_fwd + q_bwd)
        dq_ref[:, ch] = qf * (sigma * (q_fwd - q_bwd))
        kf_ref[:, ch] = fall * mm(fwd, qf * rise, TN)
        kb_ref[:, ch] = rise * mm(bwd, qf * fall, TN)
        vg_ref[:, vh] = mm(score_ref[h], oo, NN)


def final_kernel(
    flag_ref, k_ref, v_ref, cum_ref, dq_ref, kf_ref, kb_ref, vg_ref,
    kva_ref, kvl_ref, kvh_ref, qoa_ref, low_ref, high_ref, got_ref, *refs
):
    decay_refs = refs[:4]
    gk_ref, gv_ref, gd_ref = refs[4:]
    length = k_ref.shape[0]
    heads = k_ref.shape[1] // DK
    sigma = DK ** (-0.5)
    suffix = jnp.where(lower_mask(length, True), 0.0, 1.0).astype(F32)
    for h in range(heads):
        ch = head_cols(h, DK)
        vh = head_cols(h, DV)
        cum = cum_ref[:, ch]
        total = cum[length - 1 :, :]
        ahead = jnp.exp(cum)
        tail = jnp.exp(total - cum)
        kf = k_ref[:, ch].astype(F32)
        vv = v_ref[:, vh]
        qo_low, qo_high = close(flag_ref, low_ref, high_ref, got_ref, decay_refs, h)
        high = qo_high.astype(BF)
        low = qo_low.astype(BF)
        whole = jnp.exp(total)
        ends = qo_high * (whole * kvl_ref[h] + kva_ref[h])
        ends = ends + kvh_ref[h] * (whole * qo_low + qoa_ref[h])
        beyond = sigma * jnp.sum(ends, axis=0, keepdims=True)
        k_fwd = kf_ref[:, ch] + tail * mm(vv, high, NN)
        k_bwd = kb_ref[:, ch] + ahead * mm(vv, low, NN)
        gk_ref[:, ch] = sigma * (k_fwd + k_bwd)
        gv_ref[:, vh] = vg_ref[:, vh] + sigma * (mm(kf * tail, high, NT) + mm(kf * ahead, low, NT))
        change = dq_ref[:, ch] - kf * (sigma * (k_fwd - k_bwd))
        gd_ref[:, ch] = beyond + jnp.dot(
            suffix, change, precision=lax.Precision.HIGHEST, preferred_element_type=F32
        )


SMEM = pl.BlockSpec(memory_space=pltpu.SMEM)
VMEM = pl.BlockSpec(memory_space=pltpu.VMEM)


def call(kernel, outs, *args, scalars=0, flops=0, name=None):
    return pl.pallas_call(
        kernel,
        out_shape=[jax.ShapeDtypeStruct(s, d) for s, d in outs],
        in_specs=[SMEM] * scalars + [VMEM] * (len(args) - scalars),
        out_specs=[VMEM] * len(outs),
        cost_estimate=pl.CostEstimate(flops=flops or 100_000_000, transcendentals=0, bytes_accessed=1_000_000),
    )(*args)


def split_call(kernel, outs, place, pieces, array, others, tensor, axis, flops):
    def spec(shape):
        block = tuple(n // tensor if i == axis else n for i, n in enumerate(shape))
        return pl.BlockSpec(
            block, lambda r, j: tuple((j[0] ^ r) if i == axis else 0 for i in range(len(shape)))
        )

    def whole(shape):
        return pl.BlockSpec(shape, lambda r, j: (0,) * len(shape))

    def one(shape):
        return pl.BlockSpec((shape[0], 1) + shape[2:], lambda r, j: (0, array, 0, 0))

    return pl.pallas_call(
        kernel,
        out_shape=[jax.ShapeDtypeStruct(s, F32) for s in outs],
        grid_spec=pltpu.PrefetchScalarGridSpec(
            num_scalar_prefetch=1,
            grid=(tensor,),
            in_specs=[one(p.shape) for p in pieces] + [whole(o.shape) for o in others],
            out_specs=[spec(s) for s in outs],
        ),
        cost_estimate=pl.CostEstimate(flops=flops, transcendentals=0, bytes_accessed=8_000_000),
    )(place, *pieces, *others)


def combine_kernel(flag_ref, *refs, single):
    ahead, back, got, mine, theirs, under, over = refs[:7]
    ahead_out, back_out, low_out, high_out, send = refs[-5:]
    before = refs[7:-5]
    rows = ahead.shape[1]
    for h in range(ahead.shape[0]):
        got_ahead = got[h, :rows, :].astype(F32)
        got_back = got[h, rows:, :].astype(F32)
        low = before[0][h] if before else jnp.zeros_like(got_ahead)
        high = before[1][h] if before else jnp.zeros_like(got_back)

        @pl.when(flag_ref[0] == 1)
        def _():
            low_out[h] = low + under[h] * got_ahead
            high_out[h] = high
            ahead_out[h] = mine[h] * got_ahead + ahead[h]
            back_out[h] = got_back + theirs[h] * back[h]

        @pl.when(flag_ref[0] == 0)
        def _():
            low_out[h] = low
            high_out[h] = high + over[h] * got_back
            ahead_out[h] = theirs[h] * ahead[h] + got_ahead
            back_out[h] = back[h] + mine[h] * got_back

        if single:

            @pl.when(flag_ref[1] == 1)
            def _():
                send[h] = back_out[h].astype(BF)

            @pl.when(flag_ref[1] == 0)
            def _():
                send[h] = ahead_out[h].astype(BF)

        else:
            send[h, :rows, :] = ahead_out[h].astype(BF)
            send[h, rows:, :] = back_out[h].astype(BF)


def group_decays(total):
    size = lax.axis_size("sp")
    place = lax.axis_index("sp")
    steps = size.bit_length() - 1
    group, below, above = total, jnp.zeros_like(total), jnp.zeros_like(total)
    record = []
    for k in range(steps):
        upper = ((place >> k) & 1) == 1
        last = k == steps - 1
        other = jnp.zeros_like(group) if last else flip_bit(group, "sp", 1 << k)
        logs = lax.optimization_barrier((group, other, below, above))
        record.append([jnp.exp(log) for log in logs])
        below = below + jnp.where(upper, other, 0.0)
        above = above + jnp.where(upper, 0.0, other)
        group = group + other
    return record


def scan_states(ahead, back, send, decays):
    place = lax.axis_index("sp")
    steps = lax.axis_size("sp").bit_length() - 1
    state = (ahead.shape, F32)
    sums = []
    for k in range(steps - 1):
        got = flip_bit(send, "sp", 1 << k)
        single = k == steps - 2
        flags = jnp.stack([(place >> k) & 1, (place >> (k + 1)) & 1]).astype(jnp.int32)
        ahead, back, low, high, send = call(
            functools.partial(combine_kernel, single=single),
            [state] * 4 + [(ahead.shape if single else send.shape, BF)],
            flags, ahead, back, got, *decays[k], *sums,
            scalars=1,
        )
        sums = [low, high]
    got = flip_bit(send, "sp", 1 << (steps - 1))
    return sums + [got]


def close(flag_ref, low_ref, high_ref, got_ref, decay_refs, h):
    upper = (flag_ref[0] == 1).astype(F32)
    got = got_ref[h].astype(F32)
    under, over = decay_refs[2][h], decay_refs[3][h]
    return low_ref[h] + (upper * under) * got, high_ref[h] + ((1.0 - upper) * over) * got


def program(
    queries,
    key_vectors,
    values_in,
    log_decay,
    mixed_heads,
    out_proj,
    layer_input,
    cotangent,
    routes,
    route_weight,
    gate_weight,
    up_weight,
    down_weight,
):
    tokens, top = routes.shape
    seq = lax.axis_size("sp")
    tensor = lax.axis_size("tp")
    halves = seq // 2
    experts, width, units = gate_weight.shape
    all_experts = experts * seq
    cap = -(-(2 * tokens * top // all_experts) // 16) * 16
    part = width // tensor
    me = lax.axis_index("sp")
    column = lax.axis_index("tp")
    my_low = me & 1
    my_high = me >> 1
    place = column.reshape(1).astype(jnp.int32)
    groups = message_groups(seq)
    rows = experts * cap

    chosen = routes.T
    base = (((chosen // experts) - me) % seq) * rows + (chosen % experts) * cap
    slot, *messages = call(
        functools.partial(pick_kernel, experts_all=all_experts),
        [((top, tokens), jnp.int32)] + [((2, rows, part), BF)] * seq,
        place, base, chosen, route_weight.T, layer_input, cotangent,
        scalars=1,
    )
    arrived = [shift(messages[d], d) if d else messages[0] for d in range(seq)]
    pieces = []
    for group in groups:
        own = jnp.stack([arrived[d] for d in group])
        beyond = flip_bit(own, "tp", 2)
        pieces += [own, flip_bit(own, "tp", 1), beyond, flip_bit(beyond, "tp", 1)]

    heads = queries.shape[1] // DK
    state = ((heads, DV, DK), F32)
    key_shape = ((tokens, heads * DK), F32)
    value_shape = ((tokens, heads * DV), F32)
    cum, score, kv_ahead, kv_back, kv_send = call(
        early_kernel,
        [key_shape, ((heads, tokens, tokens), BF), state, state, ((heads, 2 * DV, DK), BF)],
        queries, key_vectors, values_in, log_decay,
    )
    total = cum[tokens - 1].reshape(heads, 1, DK)
    decays = group_decays(total)
    kv_sums = scan_states(kv_ahead, kv_back, kv_send, decays)
    flag = (me >> (seq.bit_length() - 2)).reshape(1).astype(jnp.int32)
    mixed = [mixed_heads] + [shift(mixed_heads, 2 * d) for d in range(1, halves)]

    flops = 2 * seq * rows * width * units
    *values, act, d_gate, d_up = call(
        functools.partial(expert_kernel, tensor=tensor, cap=cap, count=len(pieces)),
        [((len(group), rows, part), BF) for group in groups for _ in range(tensor)] + [((experts, seq * cap, units), BF)] * 3,
        place, *pieces, gate_weight.reshape(experts, tensor, part, units),
        up_weight.reshape(experts, tensor, part, units), down_weight,
        scalars=1, flops=5 * flops,
    )
    grad_gate, grad_up = split_call(
        functools.partial(rows_kernel, tensor=tensor, cap=cap),
        [gate_weight.shape, up_weight.shape],
        place, pieces, 0, [d_gate, d_up], tensor, 1, 2 * flops,
    )
    (grad_down,) = split_call(
        functools.partial(weighted_kernel, tensor=tensor, cap=cap),
        [down_weight.shape],
        place, pieces, 1, [act], tensor, 2, flops,
    )

    back = [None] * seq
    for g, group in enumerate(groups):
        value = [v.astype(F32) for v in values[tensor * g : tensor * (g + 1)]]
        away = value[2] + flip_bit(values[tensor * g + 3], "tp", 1).astype(F32)
        near = value[0] + flip_bit(values[tensor * g + 1], "tp", 1).astype(F32)
        other = flip_bit(away.astype(BF), "tp", 2).astype(F32)
        for i, d in enumerate(group):
            row = (near[i] + other[i]).astype(BF)
            back[d] = shift(row, seq - d) if d else row
    (token_part,) = call(
        join_kernel, [((tokens, part), BF)], place, slot, cotangent, *back, scalars=1
    )
    token_far = flip_bit(token_part, "tp", 2)
    token_parts = [
        token_part, flip_bit(token_part, "tp", 1),
        token_far, flip_bit(token_far, "tp", 1),
    ]

    out_bf, qo_send, qo_ahead, qo_back = call(
        functools.partial(grad_kernel, tensor=tensor),
        [((tokens, heads * DV), BF), ((heads, 2 * DV, DK), BF), state, state],
        place, *token_parts, out_proj, queries, cum,
        scalars=1, flops=2 * tokens * width * heads * DV,
    )
    qo_sums = scan_states(qo_ahead, qo_back, qo_send, decays)
    query_grad, dq, k_fwd, k_bwd, v_local, kv_low, kv_high = call(
        local_kernel,
        [key_shape, key_shape, key_shape, key_shape, value_shape, state, state],
        flag, queries, key_vectors, values_in, cum, out_bf, score, *kv_sums, *decays[-1],
        scalars=1,
    )
    key_grad, value_grad, grad_decay = call(
        final_kernel,
        [key_shape, value_shape, key_shape],
        flag, key_vectors, values_in, cum, dq, k_fwd, k_bwd, v_local,
        kv_ahead, kv_low, kv_high, qo_ahead, *qo_sums, *decays[-1],
        scalars=1,
    )

    feats = width // halves
    if halves == tensor:
        turned = lax.ppermute(
            token_part, ("sp", "tp"),
            [
                ((a * 2 + low) * tensor + b, (b * 2 + low) * tensor + a)
                for a in range(halves) for low in range(2) for b in range(tensor)
            ],
        )
        far = flip_bit(turned, "tp", 2)
        cut = [turned, flip_bit(turned, "tp", 1), far, flip_bit(far, "tp", 1)]
        stacked = jnp.stack(mixed)
        mixed = [stacked[(my_high - (column ^ r)) % halves] for r in range(tensor)]
    else:
        near = [token_parts[r] for r in range(tensor)]
        whole = jnp.zeros((tensor, tokens, part), BF)
        for r in range(tensor):
            whole = lax.dynamic_update_index_in_dim(whole, near[r], column ^ r, 0)
        whole = whole.transpose(1, 0, 2).reshape(tokens, width)
        cut = []
        for d in range(halves):
            some = lax.dynamic_slice_in_dim(whole, ((my_high + d) % halves) * feats, feats, 1)
            cut.append(shift(some, 2 * d) if d else some)
    block = lax.dot_general(
        jnp.concatenate(cut), jnp.concatenate(mixed), (((0,), (0,)), ((), ())),
        preferred_element_type=F32,
    ).reshape(2, feats // 2, -1)
    keep = jnp.where(my_low == 0, block[0], block[1])
    give = jnp.where(my_low == 0, block[1], block[0]).astype(BF)
    grad_proj = keep + flip_bit(give, "sp", 1).astype(F32)
    return (
        grad_gate,
        grad_up,
        grad_down,
        grad_proj,
        query_grad,
        key_grad,
        value_grad,
        grad_decay,
    )


def solution(mesh):
    return jax.shard_map(
        program,
        mesh=mesh,
        in_specs=(
            P("sp", "tp"),
            P("sp", "tp"),
            P("sp", "tp"),
            P("sp", "tp"),
            P("sp", "tp"),
            P("tp", None),
            P("sp", None),
            P("sp", None),
            P("sp", None),
            P("sp", None),
            P("sp", None, "tp"),
            P("sp", None, "tp"),
            P("sp", "tp", None),
        ),
        out_specs=(
            P("sp", None, "tp"),
            P("sp", None, "tp"),
            P("sp", "tp", None),
            P("sp", "tp"),
            P("sp", "tp"),
            P("sp", "tp"),
            P("sp", "tp"),
            P("sp", "tp"),
        ),
        check_vma=False,
    )
```

```python
import functools
import jax
import jax.numpy as jnp
from jax import lax
from jax.experimental import pallas as pl
from jax.experimental.pallas import tpu as pltpu
from jax.sharding import PartitionSpec as P

DK = 128
DV = 256
PARTS = 16
BF = jnp.bfloat16
F32 = jnp.float32


def flip_bit(value, axis, bit):
    size = lax.axis_size(axis)
    return lax.ppermute(value, axis, [(s, s ^ bit) for s in range(size)])


def shift(value, step):
    size = lax.axis_size("sp")
    return lax.ppermute(value, "sp", [(s, (s + step) % size) for s in range(size)])


def distances(size):
    return sorted(range(1, size), key=lambda d: abs(d - size // 2))


def message_groups(size):
    order = distances(size)
    step = max(1, size // 4)
    return [[0], order[:step], order[step : 2 * step], order[2 * step :]]


EARLY = 3


def mm(a, b, contract):
    return lax.dot_general(
        a.astype(BF), b.astype(BF), ((contract[0], contract[1]), ((), ())), preferred_element_type=F32
    )


NN = ((1,), (0,))
NT = ((1,), (1,))
TN = ((0,), (0,))


def lower_mask(length, strict=False):
    row = lax.broadcasted_iota(jnp.int32, (length, length), 0)
    col = lax.broadcasted_iota(jnp.int32, (length, length), 1)
    return row > col if strict else row >= col


def head_cols(h, width):
    return slice(h * width, (h + 1) * width)


def stacked_rows(rows, count):
    number = lax.broadcasted_iota(jnp.int32, (count, DK), 0)
    out = jnp.zeros((count, DK), F32)
    for at, row in rows.items():
        out = jnp.where(number == at, row, out)
    return out


def in_parts(row):
    first = row.astype(BF).astype(F32)
    second = (row - first).astype(BF).astype(F32)
    return stacked_rows({0: first, 1: second, 2: row - first - second}, PARTS).astype(BF)


def early_kernel(q_ref, k_ref, v_ref, ld_ref, cum_ref, score_ref, kvf_ref, kvb_ref, send_ref, logs_ref):
    length = q_ref.shape[0]
    heads = q_ref.shape[1] // DK
    sigma = DK ** (-0.5)
    tri = jnp.where(lower_mask(length), 1.0, 0.0).astype(F32)
    upper = jnp.logical_not(lower_mask(length, True))
    for h in range(heads):
        ch = head_cols(h, DK)
        cum = jnp.dot(
            tri, ld_ref[:, ch], precision=lax.Precision.HIGHEST, preferred_element_type=F32
        )
        cum_ref[:, ch] = cum
        total = cum[length - 1 :, :]
        middle = 0.5 * total
        rise = jnp.exp(cum - middle)
        fall = jnp.exp(middle - cum)
        qf = q_ref[:, ch].astype(F32)
        kf = k_ref[:, ch].astype(F32)
        ahead = mm(kf * fall, qf * rise, NT)
        behind = mm(kf * rise, qf * fall, NT)
        score_ref[h] = (jnp.where(upper, ahead, behind) * sigma).astype(BF)
        vv = v_ref[:, head_cols(h, DV)]
        ahead = mm(vv, kf * jnp.exp(total - cum), TN)
        back = mm(vv, kf * jnp.exp(cum), TN)
        kvf_ref[h] = ahead
        kvb_ref[h] = back
        send_ref[h, :DV, :] = ahead.astype(BF)
        send_ref[h, DV : 2 * DV, :] = back.astype(BF)
        send_ref[h, 2 * DV :, :] = in_parts(total)
        logs_ref[h] = stacked_rows({0: total}, 8)


def slot_kernel(base_ref, route_ref, slot_ref, *, experts_all):
    top, tokens = base_ref.shape
    names = lax.broadcasted_iota(jnp.int32, (experts_all, tokens), 0)
    hits = [route_ref[k : k + 1, :] == names for k in range(top)]
    count = functools.reduce(jnp.add, [jnp.where(hit, 1.0, 0.0) for hit in hits]).astype(BF)
    row = lax.broadcasted_iota(jnp.int32, (tokens, tokens), 0)
    col = lax.broadcasted_iota(jnp.int32, (tokens, tokens), 1)
    before = mm(count, jnp.where(row < col, 1.0, 0.0), NN)
    for k in range(top):
        rank = jnp.sum(jnp.where(hits[k], before, 0.0), axis=0, keepdims=True)
        slot_ref[k : k + 1, :] = base_ref[k : k + 1, :] + rank.astype(jnp.int32)


def picked(slot_ref, first, rows):
    top, tokens = slot_ref.shape
    numbers = first + lax.broadcasted_iota(jnp.int32, (rows, tokens), 0)
    return [slot_ref[k : k + 1, :] == numbers for k in range(top)]


def pick_kernel(place_ref, base_ref, route_ref, weight_ref, in_ref, cot_ref, *refs, experts_all):
    slot_ref, cut_ref, *outs = refs[:-2]
    own_ref, sem = refs[-2:]
    _, rows, part = outs[0].shape
    lanes = pl.ds(pl.multiple_of(place_ref[0] * part, part), part)
    copy_in = pltpu.make_async_copy(in_ref.at[:, lanes], own_ref, sem.at[0])
    copy_cot = pltpu.make_async_copy(cot_ref.at[:, lanes], cut_ref, sem.at[1])
    copy_in.start()
    copy_cot.start()
    slot_kernel(base_ref, route_ref, slot_ref, experts_all=experts_all)
    copy_in.wait()
    copy_cot.wait()
    own_in = own_ref[...]
    own_cot = cut_ref[...]
    for d, out in enumerate(outs):
        hits = picked(slot_ref, d * rows, rows)
        pick = jnp.where(functools.reduce(jnp.logical_or, hits), 1.0, 0.0).astype(BF)
        scale = functools.reduce(
            jnp.add,
            [
                jnp.sum(jnp.where(hit, weight_ref[k : k + 1, :], 0.0), axis=1, keepdims=True)
                for k, hit in enumerate(hits)
            ],
        )
        out[0] = mm(pick, own_in, NN).astype(BF)
        out[1] = (scale * mm(pick, own_cot, NN)).astype(BF)


def join_kernel(slot_ref, cot_ref, *refs):
    part_ref = refs[-1]
    rows, _ = refs[0].shape
    total = cot_ref[...].astype(F32)
    for d, ref in enumerate(refs[:-1]):
        hits = picked(slot_ref, d * rows, rows)
        pick = jnp.where(functools.reduce(jnp.logical_or, hits), 1.0, 0.0).astype(BF)
        total = total + mm(pick, ref[...], TN)
    part_ref[...] = total.astype(BF)


def piece(refs, tensor, r, array, e, cap):
    blocks = []
    for ref in refs[r::tensor]:
        for i in range(ref.shape[0]):
            blocks.append(ref[i, array, e * cap : (e + 1) * cap, :])
    return jnp.concatenate(blocks, axis=0)


def expert_kernel(place_ref, *refs, tensor, cap, count):
    pieces = refs[:count]
    gate_ref, up_ref, down_ref = refs[count : count + 3]
    values = refs[count + 3 : -3]
    act_ref, dg_ref, du_ref = refs[-3:]
    experts, _, part, _ = gate_ref.shape
    for e in range(experts):
        gate = up = d_act = None
        for r in range(tensor):
            q = place_ref[0] ^ r
            rows = piece(pieces, tensor, r, 0, e, cap)
            g = mm(rows, gate_ref[e, q], NN)
            u = mm(rows, up_ref[e, q], NN)
            lanes = pl.ds(pl.multiple_of(q * part, part), part)
            a = mm(piece(pieces, tensor, r, 1, e, cap), down_ref[e, :, lanes], NT)
            gate, up, d_act = (g, u, a) if r == 0 else (gate + g, up + u, d_act + a)
        s = 1.0 / (1.0 + jnp.exp(-gate))
        silu = gate * s
        act_ref[e] = (silu * up).astype(BF)
        dg = (d_act * up * s * (1.0 + gate * (1.0 - s))).astype(BF)
        du = (d_act * silu).astype(BF)
        dg_ref[e] = dg
        du_ref[e] = du
        for r in range(tensor):
            q = place_ref[0] ^ r
            value = (mm(dg, gate_ref[e, q], NT) + mm(du, up_ref[e, q], NT)).astype(BF)
            at = 0
            for ref in values[r::tensor]:
                for i in range(ref.shape[0]):
                    ref[i, e * cap : (e + 1) * cap, :] = value[at : at + cap, :]
                    at += cap


def rows_kernel(place_ref, *refs, tensor, cap):
    gate_out, up_out = refs[-2:]
    gate_refs, up_refs = refs[-6:-4], refs[-4:-2]
    pieces = refs[:-6]
    for r in range(tensor):

        @pl.when(pl.program_id(0) == r)
        def _():
            for e in range(gate_out.shape[0]):
                rows = piece(pieces, tensor, r, 0, e, cap)
                gate_out[e] = mm(rows, jnp.concatenate([ref[e] for ref in gate_refs], axis=0), TN)
                up_out[e] = mm(rows, jnp.concatenate([ref[e] for ref in up_refs], axis=0), TN)


def weighted_kernel(place_ref, *refs, tensor, cap):
    gd_ref = refs[-1]
    act_refs = refs[-3:-1]
    pieces = refs[:-3]
    for r in range(tensor):

        @pl.when(pl.program_id(0) == r)
        def _():
            for e in range(gd_ref.shape[0]):
                act = jnp.concatenate([ref[e] for ref in act_refs], axis=0)
                gd_ref[e] = mm(act, piece(pieces, tensor, r, 0, e, cap), TN)


def grad_kernel(place_ref, *refs, tensor):
    parts = refs[:tensor]
    w_ref, q_ref, cum_ref, o_ref, send_ref, qof_ref, qob_ref = refs[tensor:]
    length = q_ref.shape[0]
    heads = q_ref.shape[1] // DK
    part = parts[0].shape[1]
    for h in range(heads):
        ch = head_cols(h, DK)
        vh = head_cols(h, DV)
        out = None
        for r in range(tensor):
            lanes = pl.ds(pl.multiple_of((place_ref[0] ^ r) * part, part), part)
            term = mm(parts[r][...], w_ref[vh, lanes], NT)
            out = term if r == 0 else out + term
        o_ref[:, vh] = out.astype(BF)
        cum = cum_ref[:, ch]
        total = cum[length - 1 :, :]
        qf = q_ref[:, ch].astype(F32)
        ahead = mm(out, qf * jnp.exp(total - cum), TN)
        back = mm(out, qf * jnp.exp(cum), TN)
        qof_ref[h] = ahead
        qob_ref[h] = back
        send_ref[h, :DV, :] = ahead.astype(BF)
        send_ref[h, DV:, :] = back.astype(BF)


def local_kernel(
    flag_ref, q_ref, k_ref, v_ref, cum_ref, o_ref, score_ref, low_ref, high_ref, got_ref, *refs
):
    logs_ref, gq_ref, dq_ref, kf_ref, kb_ref, vg_ref, kvl_ref, kvh_ref = refs
    length = q_ref.shape[0]
    heads = q_ref.shape[1] // DK
    sigma = DK ** (-0.5)
    lower = lower_mask(length)
    for h in range(heads):
        ch = head_cols(h, DK)
        vh = head_cols(h, DV)
        cum = cum_ref[:, ch]
        total = cum[length - 1 :, :]
        middle = 0.5 * total
        rise = jnp.exp(cum - middle)
        fall = jnp.exp(middle - cum)
        qf = q_ref[:, ch].astype(F32)
        kf = k_ref[:, ch].astype(F32)
        oo = o_ref[:, vh]
        vv = v_ref[:, vh]
        pair = mm(oo, vv, NT)
        fwd = jnp.where(lower, pair, 0.0).astype(BF)
        bwd = jnp.where(lower, 0.0, pair).astype(BF)
        kv_low, kv_high = close(flag_ref, low_ref, high_ref, got_ref, logs_ref, h)
        kvl_ref[h] = kv_low
        kvh_ref[h] = kv_high
        q_fwd = rise * mm(fwd, kf * fall, NN) + jnp.exp(cum) * mm(oo, kv_low, NN)
        q_bwd = fall * mm(bwd, kf * rise, NN) + jnp.exp(total - cum) * mm(oo, kv_high, NN)
        gq_ref[:, ch] = sigma * (q_fwd + q_bwd)
        dq_ref[:, ch] = qf * (sigma * (q_fwd - q_bwd))
        kf_ref[:, ch] = fall * mm(fwd, qf * rise, TN)
        kb_ref[:, ch] = rise * mm(bwd, qf * fall, TN)
        vg_ref[:, vh] = mm(score_ref[h], oo, NN)


def final_kernel(
    flag_ref, k_ref, v_ref, cum_ref, dq_ref, kf_ref, kb_ref, vg_ref,
    kva_ref, kvl_ref, kvh_ref, qoa_ref, low_ref, high_ref, got_ref, *refs
):
    logs_ref, gk_ref, gv_ref, gd_ref = refs
    length = k_ref.shape[0]
    heads = k_ref.shape[1] // DK
    sigma = DK ** (-0.5)
    suffix = jnp.where(lower_mask(length, True), 0.0, 1.0).astype(F32)
    for h in range(heads):
        ch = head_cols(h, DK)
        vh = head_cols(h, DV)
        cum = cum_ref[:, ch]
        total = cum[length - 1 :, :]
        ahead = jnp.exp(cum)
        tail = jnp.exp(total - cum)
        kf = k_ref[:, ch].astype(F32)
        vv = v_ref[:, vh]
        qo_low, qo_high = close(flag_ref, low_ref, high_ref, got_ref, logs_ref, h)
        high = qo_high.astype(BF)
        low = qo_low.astype(BF)
        whole = jnp.exp(total)
        ends = qo_high * (whole * kvl_ref[h] + kva_ref[h])
        ends = ends + kvh_ref[h] * (whole * qo_low + qoa_ref[h])
        beyond = sigma * jnp.sum(ends, axis=0, keepdims=True)
        k_fwd = kf_ref[:, ch] + tail * mm(vv, high, NN)
        k_bwd = kb_ref[:, ch] + ahead * mm(vv, low, NN)
        gk_ref[:, ch] = sigma * (k_fwd + k_bwd)
        gv_ref[:, vh] = vg_ref[:, vh] + sigma * (mm(kf * tail, high, NT) + mm(kf * ahead, low, NT))
        change = dq_ref[:, ch] - kf * (sigma * (k_fwd - k_bwd))
        gd_ref[:, ch] = beyond + jnp.dot(
            suffix, change, precision=lax.Precision.HIGHEST, preferred_element_type=F32
        )


SMEM = pl.BlockSpec(memory_space=pltpu.SMEM)
VMEM = pl.BlockSpec(memory_space=pltpu.VMEM)


LIMITS = {"pick": 0, "early": 0, "expert": 30, "rows": 12, "weighted": 0, "join": 30, "grad": 30, "mix": 12, "local": 12, "final": 12}


def params(kind):
    return pltpu.CompilerParams(vmem_limit_bytes=LIMITS[kind] << 20 or None)


def call(kind, kernel, outs, *args, scalars=0, flops=0):
    return pl.pallas_call(
        kernel,
        out_shape=[jax.ShapeDtypeStruct(s, d) for s, d in outs],
        in_specs=[SMEM] * scalars + [VMEM] * (len(args) - scalars),
        out_specs=[VMEM] * len(outs),
        cost_estimate=pl.CostEstimate(flops=flops or 100_000_000, transcendentals=0, bytes_accessed=1_000_000),
        compiler_params=params(kind),
    )(*args)


def split_call(kind, kernel, outs, place, pieces, array, others, tensor, axis, flops):
    def spec(shape):
        block = tuple(n // tensor if i == axis else n for i, n in enumerate(shape))
        return pl.BlockSpec(
            block, lambda r, j: tuple((j[0] ^ r) if i == axis else 0 for i in range(len(shape)))
        )

    def whole(shape):
        return pl.BlockSpec(shape, lambda r, j: (0,) * len(shape))

    def one(shape):
        return pl.BlockSpec((shape[0], 1) + shape[2:], lambda r, j: (0, array, 0, 0))

    return pl.pallas_call(
        kernel,
        out_shape=[jax.ShapeDtypeStruct(s, F32) for s in outs],
        grid_spec=pltpu.PrefetchScalarGridSpec(
            num_scalar_prefetch=1,
            grid=(tensor,),
            in_specs=[one(p.shape) for p in pieces] + [whole(o.shape) for o in others],
            out_specs=[spec(s) for s in outs],
        ),
        cost_estimate=pl.CostEstimate(flops=flops, transcendentals=0, bytes_accessed=8_000_000),
        compiler_params=params(kind),
    )(place, *pieces, *others)


def combine_kernel(flag_ref, logs, ahead, back, got, *refs, single, carry, first):
    before = refs[: 0 if first else 2]
    ahead_out, back_out, low_out, high_out, send = refs[len(before) : len(before) + 5]
    rows = ahead.shape[1]
    upper = (flag_ref[0] == 1).astype(F32)
    for h in range(ahead.shape[0]):
        got_ahead = got[h, :rows, :].astype(F32)
        got_back = got[h, rows : 2 * rows, :].astype(F32)
        mine, under, over = logs[h, 0:1, :], logs[h, 2:3, :], logs[h, 3:4, :]
        theirs = logs[h, 1:2, :]
        if carry:
            sent = got[h, 2 * rows :, :].astype(F32)
            theirs = sent[0:1, :] + sent[1:2, :] + sent[2:3, :]
            number = lax.broadcasted_iota(jnp.int32, (8, DK), 0)
            full_out, next_out = refs[-2:]
            full_out[h] = jnp.where(number == 1, theirs, logs[h])
            next_out[h] = stacked_rows(
                {0: mine + theirs, 2: under + upper * theirs, 3: over + (1.0 - upper) * theirs}, 8
            )
        kept, passed = jnp.exp(mine), jnp.exp(theirs)
        low = before[0][h] if before else jnp.zeros_like(got_ahead)
        high = before[1][h] if before else jnp.zeros_like(got_back)

        @pl.when(flag_ref[0] == 1)
        def _():
            low_out[h] = low + jnp.exp(under) * got_ahead
            high_out[h] = high
            ahead_out[h] = kept * got_ahead + ahead[h]
            back_out[h] = got_back + passed * back[h]

        @pl.when(flag_ref[0] == 0)
        def _():
            low_out[h] = low
            high_out[h] = high + jnp.exp(over) * got_back
            ahead_out[h] = passed * ahead[h] + got_ahead
            back_out[h] = back[h] + kept * got_back

        if single:

            @pl.when(flag_ref[1] == 1)
            def _():
                send[h] = back_out[h].astype(BF)

            @pl.when(flag_ref[1] == 0)
            def _():
                send[h] = ahead_out[h].astype(BF)

        else:
            send[h, :rows, :] = ahead_out[h].astype(BF)
            send[h, rows : 2 * rows, :] = back_out[h].astype(BF)
            if carry:
                send[h, 2 * rows :, :] = in_parts(mine + theirs)


def scan_states(ahead, back, send, logs=None, record=None):
    place = lax.axis_index("sp")
    steps = lax.axis_size("sp").bit_length() - 1
    carry = record is None
    record = [] if carry else record
    heads = ahead.shape[0]
    state = (ahead.shape, F32)
    log_shape = ((heads, 8, DK), F32)
    sums = []
    for k in range(steps - 1):
        got = flip_bit(send, "sp", 1 << k)
        single = k == steps - 2
        flags = jnp.stack([(place >> k) & 1, (place >> (k + 1)) & 1]).astype(jnp.int32)
        ahead, back, low, high, send, *more = call(
            "mix", functools.partial(combine_kernel, single=single, carry=carry, first=k == 0),
            [state] * 4
            + [(ahead.shape if single else send.shape, BF)]
            + [log_shape] * (2 if carry else 0),
            flags, logs if carry else record[k], ahead, back, got, *sums,
            scalars=1,
        )
        if carry:
            full, logs = more
            record.append(full)
        sums = [low, high]
    got = flip_bit(send, "sp", 1 << (steps - 1))
    if carry:
        record.append(logs)
    return sums + [got], record


def close(flag_ref, low_ref, high_ref, got_ref, logs_ref, h):
    upper = (flag_ref[0] == 1).astype(F32)
    got = got_ref[h].astype(F32)
    under, over = jnp.exp(logs_ref[h, 2:3, :]), jnp.exp(logs_ref[h, 3:4, :])
    return low_ref[h] + (upper * under) * got, high_ref[h] + ((1.0 - upper) * over) * got


def program(
    queries,
    key_vectors,
    values_in,
    log_decay,
    mixed_heads,
    out_proj,
    layer_input,
    cotangent,
    routes,
    route_weight,
    gate_weight,
    up_weight,
    down_weight,
):
    tokens, top = routes.shape
    seq = lax.axis_size("sp")
    tensor = lax.axis_size("tp")
    halves = seq // 2
    experts, width, units = gate_weight.shape
    all_experts = experts * seq
    cap = -(-(2 * tokens * top // all_experts) // 16) * 16
    part = width // tensor
    me = lax.axis_index("sp")
    column = lax.axis_index("tp")
    my_low = me & 1
    my_high = me >> 1
    place = column.reshape(1).astype(jnp.int32)
    groups = message_groups(seq)
    rows = experts * cap

    chosen = routes.T
    base = (((chosen // experts) - me) % seq) * rows + (chosen % experts) * cap
    slot, own_cot, *messages = pl.pallas_call(
        functools.partial(pick_kernel, experts_all=all_experts),
        out_shape=[
            jax.ShapeDtypeStruct((top, tokens), jnp.int32),
            jax.ShapeDtypeStruct((tokens, part), BF),
        ]
        + [jax.ShapeDtypeStruct((2, rows, part), BF)] * seq,
        in_specs=[SMEM] + [VMEM] * 3 + [pl.BlockSpec(memory_space=pltpu.HBM)] * 2,
        out_specs=[VMEM] * (2 + seq),
        scratch_shapes=[pltpu.VMEM((tokens, part), BF), pltpu.SemaphoreType.DMA((2,))],
        cost_estimate=pl.CostEstimate(flops=800_000_000, transcendentals=0, bytes_accessed=0),
        compiler_params=params("pick"),
    )(place, base, chosen, route_weight.T, layer_input, cotangent)
    arrived = [shift(messages[d], d) if d else messages[0] for d in range(seq)]
    pieces = []
    for group in groups:
        own = jnp.stack([arrived[d] for d in group])
        beyond = flip_bit(own, "tp", 2)
        pieces += [own, flip_bit(own, "tp", 1), beyond, flip_bit(beyond, "tp", 1)]

    heads = queries.shape[1] // DK
    state = ((heads, DV, DK), F32)
    key_shape = ((tokens, heads * DK), F32)
    value_shape = ((tokens, heads * DV), F32)
    cum, score, kv_ahead, kv_back, kv_send, logs = call(
        "early", early_kernel,
        [
            key_shape, ((heads, tokens, tokens), BF), state, state,
            ((heads, 2 * DV + PARTS, DK), BF), ((heads, 8, DK), F32),
        ],
        queries, key_vectors, values_in, log_decay,
    )
    kv_sums, record = scan_states(kv_ahead, kv_back, kv_send, logs=logs)
    flag = (me >> (seq.bit_length() - 2)).reshape(1).astype(jnp.int32)
    mixed = [mixed_heads] + [shift(mixed_heads, 2 * d) for d in range(1, halves)]

    flops = 2 * seq * rows * width * units
    weights = (
        gate_weight.reshape(experts, tensor, part, units),
        up_weight.reshape(experts, tensor, part, units),
        down_weight,
    )
    values, units_out = [], []
    for some in (slice(0, EARLY), slice(EARLY, None)):
        taken = pieces[tensor * some.start : tensor * some.stop if some.stop else None]
        count = sum(len(group) for group in groups[some])
        *value, act, d_gate, d_up = call(
            "expert", functools.partial(expert_kernel, tensor=tensor, cap=cap, count=len(taken)),
            [((len(group), rows, part), BF) for group in groups[some] for _ in range(tensor)]
            + [((experts, count * cap, units), BF)] * 3,
            place, *taken, *weights,
            scalars=1, flops=5 * flops * count // seq,
        )
        values += value
        units_out.append((act, d_gate, d_up))
    acts, d_gates, d_ups = zip(*units_out)
    grad_gate, grad_up = split_call(
        "rows", functools.partial(rows_kernel, tensor=tensor, cap=cap),
        [gate_weight.shape, up_weight.shape],
        place, pieces, 0, [*d_gates, *d_ups], tensor, 1, 2 * flops,
    )
    (grad_down,) = split_call(
        "weighted", functools.partial(weighted_kernel, tensor=tensor, cap=cap),
        [down_weight.shape],
        place, pieces, 1, [*acts], tensor, 2, flops,
    )

    back = [None] * seq
    for g, group in enumerate(groups):
        value = [v.astype(F32) for v in values[tensor * g : tensor * (g + 1)]]
        away = value[2] + flip_bit(values[tensor * g + 3], "tp", 1).astype(F32)
        near = value[0] + flip_bit(values[tensor * g + 1], "tp", 1).astype(F32)
        other = flip_bit(away.astype(BF), "tp", 2).astype(F32)
        for i, d in enumerate(group):
            row = (near[i] + other[i]).astype(BF)
            back[d] = shift(row, seq - d) if d else row
    (token_part,) = call(
        "join", join_kernel, [((tokens, part), BF)], slot, own_cot, *back
    )
    token_far = flip_bit(token_part, "tp", 2)
    token_parts = [
        token_part, flip_bit(token_part, "tp", 1),
        token_far, flip_bit(token_far, "tp", 1),
    ]

    out_bf, qo_send, qo_ahead, qo_back = call(
        "grad", functools.partial(grad_kernel, tensor=tensor),
        [((tokens, heads * DV), BF), ((heads, 2 * DV, DK), BF), state, state],
        place, *token_parts, out_proj, queries, cum,
        scalars=1, flops=2 * tokens * width * heads * DV,
    )
    qo_sums, _ = scan_states(qo_ahead, qo_back, qo_send, record=record)
    query_grad, dq, k_fwd, k_bwd, v_local, kv_low, kv_high = call(
        "local", local_kernel,
        [key_shape, key_shape, key_shape, key_shape, value_shape, state, state],
        flag, queries, key_vectors, values_in, cum, out_bf, score, *kv_sums, record[-1],
        scalars=1,
    )
    key_grad, value_grad, grad_decay = call(
        "final", final_kernel,
        [key_shape, value_shape, key_shape],
        flag, key_vectors, values_in, cum, dq, k_fwd, k_bwd, v_local,
        kv_ahead, kv_low, kv_high, qo_ahead, *qo_sums, record[-1],
        scalars=1,
    )

    feats = width // halves
    if halves == tensor:
        turned = lax.ppermute(
            token_part, ("sp", "tp"),
            [
                ((a * 2 + low) * tensor + b, (b * 2 + low) * tensor + a)
                for a in range(halves) for low in range(2) for b in range(tensor)
            ],
        )
        far = flip_bit(turned, "tp", 2)
        cut = [turned, flip_bit(turned, "tp", 1), far, flip_bit(far, "tp", 1)]
        stacked = jnp.stack(mixed)
        mixed = [stacked[(my_high - (column ^ r)) % halves] for r in range(tensor)]
    else:
        near = [token_parts[r] for r in range(tensor)]
        whole = jnp.zeros((tensor, tokens, part), BF)
        for r in range(tensor):
            whole = lax.dynamic_update_index_in_dim(whole, near[r], column ^ r, 0)
        whole = whole.transpose(1, 0, 2).reshape(tokens, width)
        cut = []
        for d in range(halves):
            some = lax.dynamic_slice_in_dim(whole, ((my_high + d) % halves) * feats, feats, 1)
            cut.append(shift(some, 2 * d) if d else some)
    block = lax.dot_general(
        jnp.concatenate(cut), jnp.concatenate(mixed), (((0,), (0,)), ((), ())),
        preferred_element_type=F32,
    ).reshape(2, feats // 2, -1)
    keep = jnp.where(my_low == 0, block[0], block[1])
    give = jnp.where(my_low == 0, block[1], block[0]).astype(BF)
    grad_proj = keep + flip_bit(give, "sp", 1).astype(F32)
    return (
        grad_gate,
        grad_up,
        grad_down,
        grad_proj,
        query_grad,
        key_grad,
        value_grad,
        grad_decay,
    )


def solution(mesh):
    return jax.shard_map(
        program,
        mesh=mesh,
        in_specs=(
            P("sp", "tp"),
            P("sp", "tp"),
            P("sp", "tp"),
            P("sp", "tp"),
            P("sp", "tp"),
            P("tp", None),
            P("sp", None),
            P("sp", None),
            P("sp", None),
            P("sp", None),
            P("sp", None, "tp"),
            P("sp", None, "tp"),
            P("sp", "tp", None),
        ),
        out_specs=(
            P("sp", None, "tp"),
            P("sp", None, "tp"),
            P("sp", "tp", None),
            P("sp", "tp"),
            P("sp", "tp"),
            P("sp", "tp"),
            P("sp", "tp"),
            P("sp", "tp"),
        ),
        check_vma=False,
    )
```
